256 devices in a mesh: grp: 2 (over y), fs: 32 (over z, core), tp: 4 (over x).
Axes of the slice: x: 4, y: 2, z: 16, core: 2. Of those that a mesh axis runs over, the one named last changes fastest.
The devices are a block of a 4x16x16 slice.
Arguments:
- prompt: bfloat16 [24576, 2048], P(('grp', 'fs')), parts along dimension 0, may hold values from -6 to 6
- routes: int32 [24576, 4], P(('grp', 'fs')), parts along dimension 0, may hold values from 0 to 31, all different within a row; in each aligned block of 384 rows (0 to 383, 384 to 767, ...) at most 60 rows name the same one
- route_weight: float32 [24576, 4], P(('grp', 'fs')), parts along dimension 0, may hold values from 0.2 to 1
- norm_gain: float32 [2048], P('fs'), may hold values from 0.1 to 1.9
- gate_train: float32 [32, 2048, 1024], P(None, 'fs', 'tp'), may hold values from -0.4 to 0.4
- up_train: float32 [32, 2048, 1024], P(None, 'fs', 'tp'), may hold values from -0.4 to 0.4
- down_train: float32 [32, 1024, 2048], P(None, 'fs', 'tp'), may hold values from -0.07 to 0.07
Outputs:
- gate_serve: bfloat16 [64, 2048, 1024], P(('grp', 'fs'), None, 'tp'), parts along dimension 0
- up_serve: bfloat16 [64, 2048, 1024], P(('grp', 'fs'), None, 'tp'), parts along dimension 0
- down_serve: bfloat16 [64, 1024, 2048], P(('grp', 'fs'), 'tp'), parts along dimension 0
- mixed: bfloat16 [24576, 2048], P(('grp', 'fs'), 'tp'), parts along dimension 0
The draws below stay inside these ranges and needn't reach their ends.
There are 2 independent parts, one for each index of `grp`. The reference program is written for one: setup_inputs(seed, part) draws one part's arguments, and reference() takes and returns one part's arrays. A program takes and returns all parts, laid end to end along the dimension named above; an argument that names none is the same for every part. Nothing has to cross between parts.
Inputs may be any that keep to these rules, and one draw needn't show every extreme that they name: `routes`: each row names 4 different experts. Among the rows of one index of fs no expert is named more than 60 times, a bound that some block reaches on some index.
All inputs are finite; a program needn't handle non-finite values.
Results may differ from the reference program's by a relative error of at most 0.012.
Values may be sent and summed in bfloat16 or wider, within the bound.
A program may use at most 128 MiB of HBM per device.

```python
import math
import jax
import jax.numpy as jnp
import numpy as np
from jax import lax

D = 2048
FF = 1024
TOP = 4
TOK_DEV = 384
EXPERTS = 32
CAP = 60
TOKENS = 12288
N_FS = 32
N_TP = 4


def shard_levels(stream_key, extent, shards, least, top_value):
    loudness, own = 1.0, jax.random.fold_in(stream_key, 6)
    for dim, parts in shards:
        heights = jnp.exp(jax.random.uniform(jax.random.fold_in(own, dim), (parts,), jnp.float32, least / len(shards), top_value / len(shards)))
        loudness = loudness * jnp.repeat(heights, extent[dim] // parts).reshape([-1 if axis == dim else 1 for axis in range(len(extent))])
    return loudness


def deal_out(own_key, own, number, rows, number_of, top, reach, slope):
    sequence = jax.random.permutation(own_key, number_of)
    packed, common = portions_of(number_of, rows * top, reach, slope, True), portions_of(number_of, rows * top, reach, slope, False)
    places = jnp.arange(number_of)

    def named(lengths, turn):
        used = int((lengths > 0).sum())
        fixed = max(1, used // 4)
        passed = fixed + (places - fixed + turn * (used - fixed)) % max(1, number_of - fixed)
        return jnp.zeros((number_of,), jnp.int32).at[sequence[jnp.where(places < fixed, places, passed)]].set(jnp.asarray(lengths, jnp.int32))

    lengths = jnp.where(number % 4 == 0, named(packed, number // 4), named(common, number - number // 4 - 1))
    mixed = jax.random.permutation(jax.random.fold_in(own, 3), number_of)
    donor, receiver = mixed[0:number_of // 2 * 2:2], mixed[1:number_of // 2 * 2:2]
    slack = jnp.minimum(lengths[donor] - 1, reach - lengths[receiver]) // 2
    slack = jnp.where((donor == sequence[0]) | (receiver == sequence[0]) | (lengths[receiver] == 0), 0, jnp.maximum(slack, 0))
    passed = jax.random.randint(jax.random.fold_in(own, 4), (number_of // 2,), 0, 1 << 20) % (slack + 1)
    lengths = lengths.at[donor].add(-passed).at[receiver].add(passed)
    members = jnp.searchsorted(jnp.cumsum(lengths), jnp.arange(rows * top), side="right").astype(jnp.int32)
    grid = members.reshape(top, rows).T
    grid = grid[jax.random.permutation(jax.random.fold_in(own, 1), rows)]
    turn = jax.random.randint(jax.random.fold_in(own, 2), (rows, 1), 0, top)
    return jnp.take_along_axis(grid, (jnp.arange(top)[None, :] + turn) % top, axis=1)


def portions_of(count, total, limit, slope, full):
    portions = [(1 << 20) // math.isqrt(rank ** slope) + 1 for rank in range(1, count + 1)]
    largest = limit if full else min(limit, max(-(-total // count), total * portions[0] // sum(portions)))
    least = 1 if total - largest >= count - 1 else 0
    counts, rest = [largest] + [least] * (count - 1), total - largest - least * (count - 1)
    while rest > 0:
        candidates = [i for i in range(1, count) if counts[i] < largest] or [i for i in range(1, count) if counts[i] < limit]
        mass, budget = sum([portions[i] for i in candidates]), rest
        for i in candidates:
            more = min(limit - counts[i], max(1, budget * portions[i] // mass), rest)
            counts[i] = counts[i] + more
            rest = rest - more
    return np.array(counts)


def scatter_about(rng, dims, scale, limit, cuts=(), held_as=jnp.bfloat16):
    values = jax.random.normal(rng, dims, jnp.float32) * scale
    if len(cuts) > 0:
        values = shard_levels(rng, dims, cuts, -0.22, 0.18) * values
    return jnp.clip(values, min=-limit, max=limit).astype(held_as)


def setup_inputs(seed: int = 0, part: int = 0) -> dict:
    keys = jax.random.split(jax.random.key(seed), 8)
    part_splits = jax.random.split(jax.random.fold_in(keys[7], part), 8)
    prompt = scatter_about(part_splits[0], (TOKENS, D), 1.0, 6.0, ((0, 32),))
    routes_keys = jax.random.split(jax.random.fold_in(part_splits[1], 1), TOKENS // TOK_DEV)
    routes_turns = jax.random.permutation(jax.random.fold_in(part_splits[1], 3), TOKENS // TOK_DEV)
    routes = jax.vmap(lambda own, number: deal_out(jax.random.fold_in(part_splits[1], 2), own, number, TOK_DEV, EXPERTS, TOP, CAP, 1))(routes_keys, routes_turns).reshape((TOKENS, TOP))
    route_weight = jnp.clip(jnp.exp(math.log(1.0) - 1.609438 * jax.random.uniform(part_splits[2], (TOKENS, TOP), jnp.float32) ** shard_levels(part_splits[2], (TOKENS, TOP), ((0, 32),), -0.2, 0.2)), 0.2, 1.0)
    norm_gain = jnp.clip(1.0 + 0.18 * jax.random.normal(keys[3], (D,), jnp.float32), 0.1, 1.9)
    gate_train = scatter_about(keys[4], (EXPERTS, D, FF), 0.055, 0.4, ((1, 32), (2, 4)), jnp.float32)
    up_train = scatter_about(keys[5], (EXPERTS, D, FF), 0.055, 0.4, ((1, 32), (2, 4)), jnp.float32)
    down_train = scatter_about(keys[6], (EXPERTS, FF, D), 0.01, 0.07, ((1, 32), (2, 4)), jnp.float32)
    return {"prompt": prompt, "routes": routes, "route_weight": route_weight, "norm_gain": norm_gain, "gate_train": gate_train, "up_train": up_train, "down_train": down_train}


LIMIT = 7.0
ALPHA = 1.702
EPS = 1e-06

def expert_apply(rows, gate_one, up_one, down_one):
    gate_pre = jnp.dot(rows, gate_one, preferred_element_type=jnp.float32)
    up_pre = jnp.dot(rows, up_one, preferred_element_type=jnp.float32)
    gate_pre = jnp.minimum(gate_pre, LIMIT)
    up_pre = jnp.clip(up_pre, -LIMIT, LIMIT)
    hidden = ((up_pre + 1.0) * gate_pre * jax.nn.sigmoid(ALPHA * gate_pre)).astype(jnp.bfloat16)
    width = hidden.shape[1] // N_TP
    total = jnp.zeros((rows.shape[0], down_one.shape[1]), jnp.float32)
    for block in range(N_TP):
        part = jnp.dot(hidden[:, block * width:(block + 1) * width], down_one[block * width:(block + 1) * width], preferred_element_type=jnp.float32).astype(jnp.bfloat16)
        part = lax.optimization_barrier(part)
        total = total + part.astype(jnp.float32)
    return total.astype(jnp.bfloat16)

def reference(prompt, routes, route_weight, norm_gain, gate_train, up_train, down_train):
    gate_serve = (norm_gain[None, :, None] * gate_train).astype(jnp.bfloat16)
    up_serve = (norm_gain[None, :, None] * up_train).astype(jnp.bfloat16)
    down_serve = down_train.astype(jnp.bfloat16)
    values = prompt.astype(jnp.float32)
    normed = (values * lax.rsqrt(lax.optimization_barrier(jnp.mean(values * values, axis=-1, keepdims=True)) + EPS)).astype(jnp.bfloat16)
    flat_expert = routes.reshape(-1).astype(jnp.int32)
    flat_weight = route_weight.reshape(-1)
    most = N_FS * CAP
    experts = gate_serve.shape[0]

    def one_expert(carry, expert):
        chosen = flat_expert == expert
        picks = jnp.nonzero(chosen, size=most, fill_value=0)[0].astype(jnp.int32)
        live = jnp.arange(most, dtype=jnp.int32) < jnp.sum(chosen.astype(jnp.int32))
        token = (picks // TOP).astype(jnp.int32)
        rows = normed[token]
        result = expert_apply(rows, gate_serve[expert], up_serve[expert], down_serve[expert])
        scale = jnp.where(live, flat_weight[picks], 0.0).astype(jnp.float32)
        carry = carry.at[token].add(result.astype(jnp.float32) * scale[:, None])
        return (carry, None)
    start = jnp.zeros(normed.shape, jnp.float32)
    total, unused = lax.scan(one_expert, start, jnp.arange(experts, dtype=jnp.int32))
    return (gate_serve, up_serve, down_serve, total.astype(jnp.bfloat16))
```

```python
import jax
import jax.numpy as jnp
from jax import lax
from jax.sharding import Mesh
from jax.sharding import PartitionSpec as P

LIMIT = 7.0
ALPHA = 1.702
EPS = 1e-06
FS = ("z", "core")
ROWS = ("gh", "gl", "z", "core")


def shards(prompt, routes, route_weight, norm_gain, gate_train, up_train, down_train):
    bf16, f32 = jnp.bfloat16, jnp.float32
    n_tp = lax.axis_size("tp")
    k = lax.axis_index("tp")
    experts, gate_rows, ff = gate_train.shape
    down_rows, cols = down_train.shape[1:]
    gate = (norm_gain[None, :, None] * gate_train).astype(bf16)
    up = (norm_gain[None, :, None] * up_train).astype(bf16)
    both = jnp.concatenate((gate, up), axis=2)
    w = jnp.concatenate((both, down_train.astype(bf16)), axis=1)
    half = w.shape[1] // 2
    mine = lax.dynamic_slice_in_dim(w, lax.axis_index("gl") * half, half, 1)
    mine = lax.all_to_all(mine, FS, split_axis=0, concat_axis=0, tiled=True)
    wk = lax.all_gather(mine, "gl", axis=1, tiled=True)
    wf = lax.all_gather(wk, "tp", axis=0)
    tok = prompt.shape[0] // n_tp
    x = lax.dynamic_slice_in_dim(prompt, k * tok, tok, 0).astype(f32)
    x = (x * lax.rsqrt(jnp.mean(x * x, axis=-1, keepdims=True) + EPS)).astype(bf16)
    r = lax.dynamic_slice_in_dim(routes, k * tok, tok, 0)
    rw = lax.dynamic_slice_in_dim(route_weight, k * tok, tok, 0)
    hot = r[:, :, None] == jnp.arange(experts, dtype=jnp.int32)[None, None, :]
    c = jnp.sum(jnp.where(hot, rw[:, :, None], 0.0), axis=1).T
    xt = lax.all_gather(x, FS, axis=0)
    call = lax.all_to_all(c, FS, split_axis=0, concat_axis=0, tiled=True)
    n_fs = xt.shape[0]
    d = xt.shape[2]
    flat = xt.reshape(n_fs * tok, d)
    out_cols = []
    hid = []
    for t in range(n_tp):
        g = jnp.dot(flat, wf[t, :, :gate_rows, :ff].reshape(d, ff), preferred_element_type=f32)
        u = jnp.dot(flat, wf[t, :, :gate_rows, ff:].reshape(d, ff), preferred_element_type=f32)
        g = jnp.minimum(g, LIMIT)
        u = jnp.clip(u, -LIMIT, LIMIT)
        hid.append(((u + 1.0) * g * jax.nn.sigmoid(ALPHA * g)).astype(bf16))
    hidden = jnp.concatenate(hid, axis=1)
    scale = call.reshape(n_fs * tok, 1)
    for t in range(n_tp):
        down = wf[t, :, gate_rows:, :].reshape(n_fs * down_rows, cols)
        out_cols.append((scale * jnp.dot(hidden, down, preferred_element_type=f32)).astype(bf16))
    out = jnp.concatenate(out_cols, axis=1)
    summed = lax.psum_scatter(out, FS, scatter_dimension=0, tiled=True)
    mixed = lax.all_to_all(summed, "tp", split_axis=1, concat_axis=0, tiled=True)
    own = wk[:, :gate_rows].reshape(1, d, 2 * ff)
    share = n_fs // n_tp
    down_own = lax.dynamic_slice_in_dim(wf, k * share, share, 1)[:, :, gate_rows:, :]
    down_own = jnp.moveaxis(down_own.reshape(n_tp, share * down_rows, cols), 0, 1).reshape(1, share * down_rows, n_tp * cols)
    return (own[:, :, :ff], own[:, :, ff:], down_own, mixed)


def solution(mesh):
    groups, n_tp = mesh.shape["grp"], mesh.shape["tp"]
    chips = mesh.shape["fs"] // 2
    pair = 2 if groups % 2 == 0 else 1
    finer = Mesh(
        mesh.devices.reshape(groups // pair, pair, chips, 2, n_tp),
        ("gh", "gl", "z", "core", "tp"),
    )
    return jax.shard_map(
        shards,
        mesh=finer,
        in_specs=(P(ROWS), P(ROWS), P(ROWS), P(FS), P(None, FS, "tp"), P(None, FS, "tp"), P(None, FS, "tp")),
        out_specs=(P(ROWS, None, "tp"), P(ROWS, None, "tp"), P(ROWS, "tp", None), P(ROWS, "tp")),
        check_vma=False,
    )
```

```python
import functools

import jax
import jax.numpy as jnp
from jax import lax
from jax.experimental import pallas as pl
from jax.experimental.pallas import tpu as pltpu
from jax.sharding import Mesh
from jax.sharding import PartitionSpec as P

LIMIT = 7.0
ALPHA = 1.702
EPS = 1e-06
FS = ("z", "core")
ROWS = ("gh", "gl", "z", "core")
MESH = pl.DeviceIdType.MESH
f32, bf16 = jnp.float32, jnp.bfloat16


def remote(src, dst, send, recv, where):
    return pltpu.make_async_remote_copy(
        src_ref=src, dst_ref=dst, send_sem=send, recv_sem=recv, device_id=where, device_id_type=MESH
    )


def apply_and_return(
    n_z, n_tp, wf, xt, ct, out, hid, cb, sib, acc_p, acc_s, fin,
    p_send, p_recv, s_send, s_recv, b_send, b_recv, f_send, f_recv,
):
    z, core, k = lax.axis_index("z"), lax.axis_index("core"), lax.axis_index("tp")
    steps = n_z // 2
    tok, width = xt.shape[1], xt.shape[2]
    sub = tok // 2
    cols = width // n_tp
    ffq = cols // 2
    gate_rows = width // wf.shape[1]
    down_rows = wf.shape[2] - gate_rows
    sign = 1 - 2 * core
    ahead = lax.rem(z + sign + n_z, n_z)
    behind = lax.rem(z - sign + n_z, n_z)
    sibling = {"core": 1 - core}

    def chips(i):
        j = steps - i
        first = lax.rem(z + j, n_z)
        second = jnp.where(i == 0, z, lax.rem(z - j + n_z, n_z))
        return first, second

    def inner(i):
        a, b = chips(i)
        x = jnp.concatenate(
            (
                xt[pl.ds(2 * a, 2)].reshape(2 * tok, width),
                xt[pl.ds(2 * b, 2)].reshape(2 * tok, width),
            ),
            axis=0,
        )
        for t in range(n_tp):
            gu = jnp.dot(x, wf[t, :, :gate_rows, :].reshape(width, cols), preferred_element_type=f32)
            g = jnp.minimum(gu[:, :ffq], LIMIT)
            u = jnp.clip(gu[:, ffq:], -LIMIT, LIMIT)
            hid[:, t * ffq : (t + 1) * ffq] = ((u + 1.0) * g * jax.nn.sigmoid(ALPHA * g)).astype(bf16)

    def outer(i):
        eye = lax.broadcasted_iota(jnp.int32, (tok, ct.shape[2]), 0) == lax.broadcasted_iota(
            jnp.int32, (tok, ct.shape[2]), 1
        )
        scales = []
        for chip in chips(i):
            for c in range(2):
                row = ct[2 * chip + c, pl.ds(2 * z + core, 1), :]
                scales.append(jnp.sum(jnp.where(eye, row, 0.0), axis=1, keepdims=True))
        scale = jnp.concatenate(scales, axis=0)
        for t in range(n_tp):
            down = wf[t, :, gate_rows:, :].reshape(wf.shape[1] * down_rows, cols)
            part = (scale * jnp.dot(hid[...], down, preferred_element_type=f32)).astype(bf16)
            for w in range(2):
                for c in range(2):
                    at = (2 * w + c) * tok
                    cb[i, w, c, :, t * cols : (t + 1) * cols] = part[at : at + tok]

    def to_sibling(i, w):
        return remote(cb.at[i, w, 1 - core], sib.at[i, w], b_send.at[i, w], b_recv.at[i, w], sibling)

    def hop_p(h, q):
        rows = pl.ds(q * sub, sub)
        return remote(
            acc_p.at[h, rows], acc_p.at[h + 1, rows], p_send.at[h, q], p_recv.at[h + 1, q], {"z": ahead}
        )

    def hop_s(h, q):
        rows = pl.ds(q * sub, sub)
        return remote(
            acc_s.at[h, rows], acc_s.at[h + 1, rows], s_send.at[h, q], s_recv.at[h + 1, q], {"z": behind}
        )

    def local(h, w, rows):
        return cb[h, w, core, rows, :].astype(f32) + sib[h, w, rows, :].astype(f32)

    def combine(h, q):
        rows = pl.ds(q * sub, sub)
        prim = jnp.where(h == 0, 0, core)

        @pl.when(h == 0)
        def _():
            acc_p[h, rows, :] = local(h, prim, rows).astype(bf16)

        @pl.when(h > 0)
        def _():
            hop_p(h - 1, q).wait_recv()
            acc_p[h, rows, :] = (local(h, prim, rows) + acc_p[h, rows, :].astype(f32)).astype(bf16)

        hop_p(h, q).start()

        @pl.when(h == 1)
        def _():
            acc_s[h, rows, :] = local(h, 1 - core, rows).astype(bf16)

        @pl.when(h > 1)
        def _():
            hop_s(h - 1, q).wait_recv()
            acc_s[h, rows, :] = (local(h, 1 - core, rows) + acc_s[h, rows, :].astype(f32)).astype(bf16)

        @pl.when(h > 0)
        def _():
            hop_s(h, q).start()

    def sib_in(i):
        for w in range(2):
            to_sibling(i, w).wait_recv()

    def body(i, carry):
        @pl.when(i > 0)
        def _():
            sib_in(i - 1)
            combine(i - 1, 0)

        inner(i)

        @pl.when(i > 0)
        def _():
            combine(i - 1, 1)

        outer(i)
        for w in range(2):
            to_sibling(i, w).start()
        return carry

    lax.fori_loop(0, steps, body, 0)
    sib_in(steps - 1)
    combine(steps - 1, 0)
    combine(steps - 1, 1)

    def to_tp(t):
        return remote(
            fin.at[t], out.at[pl.ds(pl.multiple_of(k * tok, tok), tok)], f_send.at[t], f_recv.at[k], {"tp": t}
        )

    for q in range(2):
        rows = pl.ds(q * sub, sub)
        hop_p(steps - 1, q).wait_recv()
        hop_s(steps - 1, q).wait_recv()
        total = (
            local(0, 1, rows)
            + acc_p[steps, rows, :].astype(f32)
            + acc_s[steps, rows, :].astype(f32)
        ).astype(bf16)
        for t in range(n_tp):
            fin[t, rows, :] = total[:, t * cols : (t + 1) * cols]
    for step in range(1, n_tp):
        to_tp(lax.rem(k + step, n_tp)).start()
    out[pl.ds(pl.multiple_of(k * tok, tok), tok), :] = fin[k]

    def drain(h, carry):
        for q in range(2):
            hop_p(h, q).wait_send()

            @pl.when(h > 0)
            def _():
                hop_s(h, q).wait_send()

        for w in range(2):
            to_sibling(h, w).wait_send()
        return carry

    lax.fori_loop(0, steps, drain, 0)
    for step in range(1, n_tp):
        t = lax.rem(k + step, n_tp)
        to_tp(t).wait_send()
        back = lax.rem(k + n_tp - step, n_tp)
        remote(
            fin.at[k], out.at[pl.ds(pl.multiple_of(back * tok, tok), tok)], f_send.at[t], f_recv.at[back], {"tp": t}
        ).wait_recv()


def apply_scratch(n_z, n_tp, n_fs, tok, width):
    steps = n_z // 2
    dma = pltpu.SemaphoreType.DMA
    return [
        pltpu.VMEM((4 * tok, width // 2), bf16),
        pltpu.VMEM((steps, 2, 2, tok, width), bf16),
        pltpu.VMEM((steps, 2, tok, width), bf16),
        pltpu.VMEM((steps + 1, tok, width), bf16),
        pltpu.VMEM((steps + 1, tok, width), bf16),
        pltpu.VMEM((n_tp, tok, width // n_tp), bf16),
        dma((steps, 2)), dma((steps + 1, 2)), dma((steps, 2)), dma((steps + 1, 2)),
        dma((steps, 2)), dma((steps, 2)), dma((n_tp,)), dma((n_tp,)),
    ]


def bring(
    n_z, n_tp, n_gl, w, xq, cq, wf, xt, ct, tbp, tbs,
    zp_send, zp_recv, zs_send, zs_recv, fz_send, wz_recv, y_send, y_recv, x_send, x_recv, r_send, r_recv,
    tp_send, tp_recv, ts_send, ts_recv, tb_send, tb_recv, l_sem, ws_send, ws_recv,
):
    z, core, k, p = (lax.axis_index(a) for a in ("z", "core", "tp", "gl"))
    top = n_z // 2
    me = 2 * z + core
    sign = 1 - 2 * core
    half = w.shape[1] // n_gl
    sub = xq.shape[0] // 2
    steps = {True: sign, False: -sign}
    length = {True: top, False: top - 1}
    transit = {True: tbp, False: tbs}
    z_send = {True: zp_send, False: zs_send}
    z_recv = {True: zp_recv, False: zs_recv}
    sibling = {"core": 1 - core}

    def chip(v):
        return lax.rem(z + v + 2 * n_z, n_z)

    def rows(q):
        return pl.ds(pl.multiple_of(q * half, half), half)

    def pair(zs):
        return pl.ds(2 * zs, 2)

    def tri(prim, h, j):
        return h * length[prim] - h * (h - 1) // 2 + j - 1

    def landed(prim, h, j):
        return transit[prim].at[tri(prim, h, j) - length[prim]]

    def z_move(prim, h, j):
        step = steps[prim]
        src = w.at[pair(chip(step * j)), rows(p)] if h == 0 else landed(prim, h, j)
        return remote(
            src, landed(prim, h + 1, j - 1), z_send[prim].at[tri(prim, h, j)],
            z_recv[prim].at[tri(prim, h + 1, j - 1)], {"z": chip(step)},
        )

    def z_wait(prim, h, j):
        here = landed(prim, h, j)
        at = tri(prim, h, j)
        remote(here, here, z_send[prim].at[at], z_recv[prim].at[at], {"z": chip(steps[prim])}).wait_recv()

    def z_final(prim, h, c2):
        step = steps[prim]
        src = w.at[2 * chip(step) + c2, rows(p)] if h == 0 else landed(prim, h, 1).at[c2]
        slot = 2 * chip(-step * h) + core
        return remote(
            src, wf.at[k, slot, rows(p)], fz_send.at[0 if prim else 1, h, c2], wz_recv.at[slot],
            {"z": chip(step), "core": c2},
        )

    def to_pair(zs, q):
        return remote(
            wf.at[k, pair(zs), rows(q)], wf.at[k, pair(zs), rows(q)], y_send.at[zs], y_recv.at[zs], {"gl": 1 - p}
        )

    def x_move(d, slot, zs, q):
        return remote(
            wf.at[slot, pair(zs), rows(q)], wf.at[slot, pair(zs), rows(q)], x_send.at[d, zs, q],
            x_recv.at[d, zs, q], {"tp": lax.rem(k + (1, n_tp - 1)[d], n_tp)},
        )

    def x_from(d):
        return lax.rem(k + (n_tp - 1, 1)[d], n_tp)

    def x_both(zs, q):
        x_move(0, k, zs, q).start()
        x_move(1, k, zs, q).start()

    def x_pass(d, slot, zs, q):
        return remote(
            wf.at[slot, pair(zs), rows(q)], wf.at[slot, pair(zs), rows(q)], r_send.at[zs, q], r_recv.at[zs, q],
            {"tp": lax.rem(k + (1, n_tp - 1)[d], n_tp)},
        )

    def relay(zs, q):
        if n_gl == 1:
            x_move(0, x_from(0), zs, q).wait_recv()
            x_pass(0, x_from(0), zs, q).start()
            return
        for d in range(2):

            @pl.when(q == d)
            def _():
                x_move(d, x_from(d), zs, d).wait_recv()
                x_pass(d, x_from(d), zs, d).start()

    def chips_at(level):
        if level == 0:
            return [z]
        if level == top:
            return [chip(top)]
        return [chip(-level), chip(level)]

    def arrive(level):
        for zs in chips_at(level):
            for c2 in range(2):
                slot = 2 * zs + c2
                here = wf.at[k, slot, rows(p)]
                remote(here, here, fz_send.at[0, 0, c2], wz_recv.at[slot], sibling).wait_recv()
            if n_gl == 2:
                to_pair(zs, p).start()
            x_both(zs, p)

    def other_half(level):
        if n_gl == 2:
            for zs in chips_at(level):
                to_pair(zs, 1 - p).wait_recv()
                x_both(zs, 1 - p)

    def forward(level, first, last):
        def one(j, carry):
            for prim in (True, False):

                @pl.when(j <= length[prim] - level)
                def _():
                    if level > 0:
                        z_wait(prim, level, j)
                    z_move(prim, level, j).start()

            return carry

        if first < last:
            lax.fori_loop(first, last, one, 0)

    def deliver(level):
        for prim in (True, False):
            if level < length[prim]:
                if level > 0:
                    z_wait(prim, level, 1)
                for c2 in range(2):
                    z_final(prim, level, c2).start()

    def part(ref, slot, q):
        return ref.at[slot, pl.ds(q * sub, sub)]

    def token(slot, q):
        return ct.at[slot] if q == 2 else part(xt, slot, q)

    def mine(q):
        return cq if q == 2 else xq.at[pl.ds(q * sub, sub)]

    t_send = {True: tp_send, False: ts_send}
    t_recv = {True: tp_recv, False: ts_recv}

    def t_move(prim, h, q):
        step = steps[prim]
        slot = 2 * chip(-step * h) + core
        return remote(
            mine(q) if h == 0 else token(slot, q), token(slot, q), t_send[prim].at[h, q],
            t_recv[prim].at[h + 1, q], {"z": chip(step)},
        )

    def t_wait(prim, h, q):
        here = token(2 * chip(-steps[prim] * h) + core, q)
        remote(here, here, t_send[prim].at[0, q], t_recv[prim].at[h, q], sibling).wait_recv()

    def t_sibling(zs, q, own=False):
        slot = 2 * zs + core
        return remote(mine(q) if own else token(slot, q), token(slot, q), tb_send.at[zs, q], tb_recv.at[zs, q], sibling)

    def t_own(q):
        return pltpu.make_async_copy(mine(q), token(me, q), l_sem.at[1 + q])

    def tokens_out():
        for q in (2, 0, 1):
            for prim in (True, False):
                if length[prim] > 0:
                    t_move(prim, 0, q).start()
        for q in (2, 0, 1):
            t_sibling(z, q, True).start()
            t_own(q).start()

    def tokens_at(h):
        for q in (2, 0, 1):
            for prim in (True, False):
                if h <= length[prim]:
                    t_wait(prim, h, q)
                    if h < length[prim]:
                        t_move(prim, h, q).start()
                    t_sibling(chip(-steps[prim] * h), q).start()

    def own_block():
        return pltpu.make_async_copy(w.at[me], wf.at[k, me], l_sem.at[0])

    def sib_block(sender):
        return remote(w.at[2 * z + 1 - core], wf.at[k, sender], ws_send, ws_recv, sibling)

    settled = max(top - 4, 0)
    late = []
    for level in range(settled + 1, top + 1):
        late += [(level, 0)] + ([(level, 1)] if n_gl == 2 else [])

    def one_late():
        if late:
            level, turn = late.pop(0)
            for zs in chips_at(level):
                relay(zs, lax.rem(p + turn, n_gl))

    own_block().start()
    sib_block(me).start()
    deliver(0)
    forward(0, 2, top + 1)
    own_block().wait()
    sib_block(me + 1 - 2 * core).wait_recv()
    for q in range(n_gl):
        x_both(z, q)
    if top - 2 < 1:
        tokens_out()
    for level in range(1, top + 1):
        arrive(level)
        deliver(level)
        if level == 1:
            for q in range(n_gl):
                relay(z, q)
        elif level - 1 <= settled and n_gl == 2:
            for zs in chips_at(level - 1):
                relay(zs, 1 - p)
        forward(level, 2, min(4, top - level + 1))
        if level < top:
            other_half(level)
        if level <= settled:
            for zs in chips_at(level):
                relay(zs, p)
        forward(level, 4, top - level + 1)
        if level == top - 2:
            tokens_out()
            one_late()
        if level == top:
            one_late()
    for h in range(1, top + 1):
        tokens_at(h)
        if h == 1:
            other_half(top)
            if settled + 1 == top:
                pass
        one_late()
    while late:
        one_late()

    def settle(zs, carry):
        @pl.when(zs != z)
        def _():
            pass

        if n_gl == 2:
            x_move(0, x_from(0), zs, 1).wait_recv()
        x_move(1, x_from(1), zs, 0).wait_recv()
        for q in range(n_gl):
            x_pass(q, lax.rem(k + 2, n_tp), zs, q).wait_recv()
        for q in range(3):
            here = token(2 * zs + 1 - core, q)
            remote(here, here, tb_send.at[zs, q], tb_recv.at[zs, q], sibling).wait_recv()
        return carry

    lax.fori_loop(0, n_z, settle, 0)
    for q in range(3):
        t_own(q).wait()

    def drain():
        sib_block(me).wait_send()

        def by_chip(zs, carry):
            for q in range(n_gl):
                x_move(0, k, zs, q).wait_send()
                x_move(1, k, zs, q).wait_send()
                x_pass(0, k, zs, q).wait_send()
            if n_gl == 2:

                @pl.when(zs != z)
                def _():
                    to_pair(zs, p).wait_send()

            for q in range(3):
                t_sibling(zs, q).wait_send()
            return carry

        lax.fori_loop(0, n_z, by_chip, 0)
        for prim in (True, False):
            for h in range(length[prim]):
                for c2 in range(2):
                    z_final(prim, h, c2).wait_send()
                for q in range(3):
                    t_move(prim, h, q).wait_send()

                def moved(j, carry):
                    z_move(prim, h, j).wait_send()
                    return carry

                if length[prim] - h >= 2:
                    lax.fori_loop(2, length[prim] - h + 1, moved, 0)

    return drain


def bring_scratch(n_z, n_tp, n_gl, w, xq, cq):
    top, n_fs = n_z // 2, 2 * n_z
    dma = pltpu.SemaphoreType.DMA
    prim, sec = top * (top + 1) // 2, top * (top - 1) // 2
    half = w[1] // n_gl
    return [
        pltpu.VMEM((n_tp, n_fs) + w[1:], bf16),
        pltpu.VMEM((n_fs,) + xq, bf16),
        pltpu.VMEM((n_fs,) + cq, f32),
        pltpu.VMEM((prim - top, 2, half, w[2]), bf16),
        pltpu.VMEM((max(sec - top + 1, 1), 2, half, w[2]), bf16),
        dma((prim,)), dma((prim,)), dma((max(sec, 1),)), dma((max(sec, 1),)),
        dma((2, top, 2)), dma((n_fs,)), dma((n_z,)), dma((n_z,)),
        dma((2, n_z, n_gl)), dma((2, n_z, n_gl)), dma((n_z, n_gl)), dma((n_z, n_gl)),
        dma((top, 3)), dma((top + 1, 3)), dma((top, 3)), dma((top + 1, 3)),
        dma((n_z, 3)), dma((n_z, 3)), dma((4,)), dma(()), dma(()),
    ]


def whole_kernel(n_z, n_tp, n_gl, n_bring, w, xq, cq, gate_out, up_out, down_out, mixed_out, *scratch):
    z, core, k, p = (lax.axis_index(a) for a in ("z", "core", "tp", "gl"))
    barrier = pltpu.get_barrier_semaphore()
    peers = [{"z": lax.rem(z + d, n_z), "core": c} for d in (1, n_z - 1) for c in range(2)]
    peers += [{"core": 1 - core}] + [{"tp": lax.rem(k + step, n_tp)} for step in range(1, n_tp)]
    if n_gl == 2:
        peers += [{"gl": 1 - p}]
    for peer in peers:
        pl.semaphore_signal(barrier, inc=1, device_id=peer, device_id_type=MESH)
    pl.semaphore_wait(barrier, len(peers))
    for_bring, for_apply, out_sem = scratch[:n_bring], scratch[n_bring:-1], scratch[-1]
    wf, xt, ct = for_bring[:3]
    drain = bring(n_z, n_tp, n_gl, w, xq, cq, *for_bring)
    gate_rows, ffq = gate_out.shape[1:]
    share, cols = down_out.shape[0], wf.shape[3]
    outs = [
        pltpu.make_async_copy(wf.at[k, :, :gate_rows, :ffq], gate_out, out_sem.at[0]),
        pltpu.make_async_copy(wf.at[k, :, :gate_rows, ffq:], up_out, out_sem.at[1]),
    ]
    for t in range(n_tp):
        outs.append(
            pltpu.make_async_copy(
                wf.at[t, pl.ds(k * share, share), gate_rows:, :],
                down_out.at[:, :, t * cols : (t + 1) * cols],
                out_sem.at[2 + t],
            )
        )
    for copy in outs:
        copy.start()
    apply_and_return(n_z, n_tp, wf, xt, ct, mixed_out, *for_apply)
    for copy in outs:
        copy.wait()
    drain()


def shards(prompt, routes, route_weight, norm_gain, gate_train, up_train, down_train):
    n_tp, n_z, n_gl = lax.axis_size("tp"), lax.axis_size("z"), lax.axis_size("gl")
    n_fs = 2 * n_z
    k = lax.axis_index("tp")
    experts, gate_rows, ffq = gate_train.shape
    down_rows, cols = down_train.shape[1:]
    gate = (norm_gain[None, :, None] * gate_train).astype(bf16)
    up = (norm_gain[None, :, None] * up_train).astype(bf16)
    both = jnp.concatenate((gate, up), axis=2)
    w = jnp.concatenate((both, down_train.astype(bf16)), axis=1)
    tok = prompt.shape[0] // n_tp
    x = lax.dynamic_slice_in_dim(prompt, k * tok, tok, 0).astype(f32)
    x = (x * lax.rsqrt(jnp.mean(x * x, axis=-1, keepdims=True) + EPS)).astype(bf16)
    r = lax.dynamic_slice_in_dim(routes, k * tok, tok, 0)
    rw = lax.dynamic_slice_in_dim(route_weight, k * tok, tok, 0)
    hot = r[:, :, None] == jnp.arange(experts, dtype=jnp.int32)[None, None, :]
    c = jnp.sum(jnp.where(hot, rw[:, :, None], 0.0), axis=1).T
    c = jnp.pad(c, ((0, 0), (0, -tok % 128)))
    d = x.shape[1]
    share = n_fs // n_tp
    vmem = pl.BlockSpec(memory_space=pltpu.VMEM)
    hbm = pl.BlockSpec(memory_space=pl.ANY)
    for_bring = bring_scratch(n_z, n_tp, n_gl, w.shape, x.shape, c.shape)
    gate_own, up_own, down_own, mixed = pl.pallas_call(
        functools.partial(whole_kernel, n_z, n_tp, n_gl, len(for_bring)),
        out_shape=(
            jax.ShapeDtypeStruct((n_fs, gate_rows, ffq), bf16),
            jax.ShapeDtypeStruct((n_fs, gate_rows, ffq), bf16),
            jax.ShapeDtypeStruct((share, down_rows, n_tp * cols), bf16),
            jax.ShapeDtypeStruct((tok * n_tp, cols), bf16),
        ),
        in_specs=[vmem] * 3,
        out_specs=(hbm, hbm, hbm, vmem),
        scratch_shapes=for_bring
        + apply_scratch(n_z, n_tp, n_fs, tok, d)
        + [pltpu.SemaphoreType.DMA((2 + n_tp,))],
        compiler_params=pltpu.CompilerParams(
            collective_id=0, has_side_effects=True, vmem_limit_bytes=67043328
        ),
    )(w, x, c)
    return (
        gate_own.reshape(1, d, ffq),
        up_own.reshape(1, d, ffq),
        down_own.reshape(1, share * down_rows, n_tp * cols),
        mixed,
    )


def solution(mesh):
    groups, n_tp = mesh.shape["grp"], mesh.shape["tp"]
    chips = mesh.shape["fs"] // 2
    pair = 2 if groups % 2 == 0 else 1
    finer = Mesh(
        mesh.devices.reshape(groups // pair, pair, chips, 2, n_tp),
        ("gh", "gl", "z", "core", "tp"),
    )
    return jax.shard_map(
        shards,
        mesh=finer,
        in_specs=(P(ROWS), P(ROWS), P(ROWS), P(FS), P(None, FS, "tp"), P(None, FS, "tp"), P(None, FS, "tp")),
        out_specs=(P(ROWS, None, "tp"), P(ROWS, None, "tp"), P(ROWS, "tp", None), P(ROWS, "tp")),
        check_vma=False,
    )
```

```python
import functools

import jax
import jax.numpy as jnp
from jax import lax
from jax.experimental import pallas as pl
from jax.experimental.pallas import tpu as pltpu
from jax.sharding import Mesh
from jax.sharding import PartitionSpec as P

LIMIT = 7.0
ALPHA = 1.702
EPS = 1e-06
FS = ("z", "core")
ROWS = ("gh", "gl", "z", "core")
MESH = pl.DeviceIdType.MESH
f32, bf16 = jnp.float32, jnp.bfloat16


def remote(src, dst, send, recv, where):
    return pltpu.make_async_remote_copy(
        src_ref=src, dst_ref=dst, send_sem=send, recv_sem=recv, device_id=where, device_id_type=MESH
    )


def apply_and_return(
    n_z, n_tp, wf, xt, ct, out, hid, cb, sib, acc_p, acc_s, fin,
    p_send, p_recv, s_send, s_recv, b_send, b_recv, f_send, f_recv,
):
    z, core, k = lax.axis_index("z"), lax.axis_index("core"), lax.axis_index("tp")
    steps = n_z // 2
    tok, width = xt.shape[1], xt.shape[2]
    sub = tok // 2
    cols = width // n_tp
    ffq = cols // 2
    gate_rows = width // wf.shape[1]
    down_rows = wf.shape[2] - gate_rows
    sign = 1 - 2 * core
    ahead = lax.rem(z + sign + n_z, n_z)
    behind = lax.rem(z - sign + n_z, n_z)
    sibling = {"core": 1 - core}

    def chips(i):
        j = steps - i
        return lax.rem(z + j, n_z), lax.rem(z - j + n_z, n_z)

    def inner(some):
        x = jnp.concatenate([xt[pl.ds(2 * chip, 2)].reshape(2 * tok, width) for chip in some], axis=0)
        count = x.shape[0]
        for t in range(n_tp):
            gu = jnp.dot(x, wf[t, :, :gate_rows, :].reshape(width, cols), preferred_element_type=f32)
            g = jnp.minimum(gu[:, :ffq], LIMIT)
            u = jnp.clip(gu[:, ffq:], -LIMIT, LIMIT)
            hid[:count, t * ffq : (t + 1) * ffq] = ((u + 1.0) * g * jax.nn.sigmoid(ALPHA * g)).astype(bf16)

    def outer(some, places):
        count = 2 * tok * len(some)
        eye = lax.broadcasted_iota(jnp.int32, (tok, ct.shape[2]), 0) == lax.broadcasted_iota(
            jnp.int32, (tok, ct.shape[2]), 1
        )
        scales = []
        for chip in some:
            for c in range(2):
                row = ct[2 * chip + c, pl.ds(2 * z + core, 1), :]
                scales.append(jnp.sum(jnp.where(eye, row, 0.0), axis=1, keepdims=True))
        scale = jnp.concatenate(scales, axis=0)
        for t in range(n_tp):
            down = wf[t, :, gate_rows:, :].reshape(wf.shape[1] * down_rows, cols)
            part = (scale * jnp.dot(hid[:count, :], down, preferred_element_type=f32)).astype(bf16)
            for n, (i, w) in enumerate(places):
                for c in range(2):
                    at = (2 * n + c) * tok
                    cb[i, w, c, :, t * cols : (t + 1) * cols] = part[at : at + tok]

    def b_slot(i, w):
        return steps * w if isinstance(i, int) and i == 0 else i

    def to_sibling(i, w):
        return remote(cb.at[i, w, 1 - core], sib.at[i, w], b_send, b_recv.at[b_slot(i, w)], sibling)

    def hop_p(h, q):
        rows = pl.ds(q * sub, sub)
        return remote(
            acc_p.at[h, rows], acc_p.at[h + 1, rows], p_send, p_recv.at[h, q], {"z": ahead}
        )

    def hop_s(h, q):
        rows = pl.ds(q * sub, sub)
        return remote(
            acc_s.at[h, rows], acc_s.at[h + 1, rows], s_send, s_recv.at[h - 1, q], {"z": behind}
        )

    def local(h, w, rows):
        return cb[h, w, core, rows, :].astype(f32) + sib[h, w, rows, :].astype(f32)

    def combine_p(h, q):
        rows = pl.ds(q * sub, sub)
        prim = jnp.where(h == 0, 0, core)

        @pl.when(h == 0)
        def _():
            acc_p[h, rows, :] = local(h, prim, rows).astype(bf16)

        @pl.when(h > 0)
        def _():
            hop_p(h - 1, q).wait_recv()
            acc_p[h, rows, :] = (local(h, prim, rows) + acc_p[h, rows, :].astype(f32)).astype(bf16)

        hop_p(h, q).start()

    def combine_s(h, q):
        rows = pl.ds(q * sub, sub)

        @pl.when(h == 1)
        def _():
            acc_s[h, rows, :] = local(h, 1 - core, rows).astype(bf16)

        @pl.when(h > 1)
        def _():
            hop_s(h - 1, q).wait_recv()
            acc_s[h, rows, :] = (local(h, 1 - core, rows) + acc_s[h, rows, :].astype(f32)).astype(bf16)

        hop_s(h, q).start()

    def sib_in(i):
        remote(sib.at[i], sib.at[i], b_send, b_recv.at[i], sibling).wait_recv()

    def sib_out(i):
        for w in range(2):
            to_sibling(i, w).start()

    def body(i, carry):
        sib_in(i)
        combine_s(i, 0)

        @pl.when(i == 1)
        def _():
            combine_s(i, 1)
            to_sibling(0, 0).wait_recv()

        combine_p(i - 1, 0)

        @pl.when(i == 1)
        def _():
            combine_p(i - 1, 1)

        inner(chips(i + 1))

        @pl.when(i > 1)
        def _():
            combine_s(i, 1)
            combine_p(i - 1, 1)

        outer(chips(i + 1), [(i + 1, 0), (i + 1, 1)])
        sib_out(i + 1)
        return carry

    def one_chip(chip, w):
        inner([chip])
        outer([chip], [(0, w)])
        to_sibling(0, w).start()

    def to_tp(t, q):
        rows = pl.ds(q * sub, sub)
        at = pl.multiple_of(k * tok + q * sub, sub)
        return remote(fin.at[t, rows], out.at[pl.ds(at, sub)], f_send, f_recv, {"tp": t})

    def sent(ref, sem):
        remote(ref, ref, sem, sem, sibling).wait_send()

    def first():
        one_chip(z, 1)

    def second():
        inner(chips(1))

    def third():
        outer(chips(1), [(1, 0), (1, 1)])
        sib_out(1)

    def rest(drain_bring):
        one_chip(lax.rem(z + steps, n_z), 0)
        lax.fori_loop(1, steps - 1, body, 0)
        last = steps - 1
        sib_in(last)
        if last == 1:
            to_sibling(0, 0).wait_recv()
        for q in range(2):
            combine_s(last, q)
            combine_p(last - 1, q)
        for q in range(2):
            combine_p(last, q)
        to_sibling(0, 1).wait_recv()
        drain_bring()
        sent(sib, b_send)
        for q in range(2):
            rows = pl.ds(q * sub, sub)
            hop_p(steps - 1, q).wait_recv()
            hop_s(steps - 1, q).wait_recv()
            total = (
                local(0, 1, rows)
                + acc_p[steps, rows, :].astype(f32)
                + acc_s[steps, rows, :].astype(f32)
            ).astype(bf16)
            for t in range(n_tp):
                fin[t, rows, :] = total[:, t * cols : (t + 1) * cols]
            for step in (2, 1, 3):
                to_tp(lax.rem(k + step, n_tp), q).start()
            out[pl.ds(pl.multiple_of(k * tok + q * sub, sub), sub), :] = fin[k, rows, :]
        sent(acc_p.at[pl.ds(0, steps)], p_send)
        sent(acc_s.at[pl.ds(0, steps - 1)], s_send)
        peers = fin.at[pl.ds(0, n_tp - 1)]
        sent(peers, f_send)
        remote(peers, peers, f_send, f_recv, sibling).wait_recv()

    return first, second, third, rest


def apply_scratch(n_z, n_tp, n_fs, tok, width):
    steps = n_z // 2
    dma = pltpu.SemaphoreType.DMA
    return [
        pltpu.VMEM((4 * tok, width // 2), bf16),
        pltpu.VMEM((steps, 2, 2, tok, width), bf16),
        pltpu.VMEM((steps, 2, tok, width), bf16),
        pltpu.VMEM((steps + 1, tok, width), bf16),
        pltpu.VMEM((steps + 1, tok, width), bf16),
        pltpu.VMEM((n_tp, tok, width // n_tp), bf16),
        dma(()), dma((steps, 2)), dma(()), dma((steps - 1, 2)), dma(()), dma((steps + 1,)), dma(()), dma(()),
    ]


def bring(
    n_z, n_tp, n_gl, prepare, first, second, third, w, xq, cq, wf, xt, ct, tbp, tbs,
    zp_send, zp_recv, zs_send, zs_recv, fz_send, wz_recv, y_send, y_recv, x_send, x_recv, r_send,
    t_send, tp_recv, ts_recv, tb_send, tb_recv, l_sem, ws_send, ws_recv,
):
    z, core, k, p = (lax.axis_index(a) for a in ("z", "core", "tp", "gl"))
    top = n_z // 2
    me = 2 * z + core
    sign = 1 - 2 * core
    half = w.shape[1] // n_gl
    sub = xq.shape[0] // 2
    steps = {True: sign, False: -sign}
    length = {True: top, False: top - 1}
    transit = {True: tbp, False: tbs}
    z_send = {True: zp_send, False: zs_send}
    z_recv = {True: zp_recv, False: zs_recv}
    sibling = {"core": 1 - core}

    def chip(v):
        return lax.rem(z + v + 2 * n_z, n_z)

    def rows(q):
        return pl.ds(pl.multiple_of(q * half, half), half)

    def pair(zs):
        return pl.ds(2 * zs, 2)

    def tri(prim, h, j):
        return h * length[prim] - h * (h - 1) // 2 + j - 1

    def landed(prim, h, j):
        return transit[prim].at[tri(prim, h, j) - length[prim]]

    def z_move(prim, h, j):
        step = steps[prim]
        src = w.at[pair(chip(step * j)), rows(p)] if h == 0 else landed(prim, h, j)
        return remote(
            src, landed(prim, h + 1, j - 1), z_send[prim],
            z_recv[prim].at[tri(prim, h + 1, j - 1) - length[prim]], {"z": chip(step)},
        )

    def z_wait(prim, h, j):
        here = landed(prim, h, j)
        at = tri(prim, h, j) - length[prim]
        remote(here, here, z_send[prim], z_recv[prim].at[at], {"z": chip(steps[prim])}).wait_recv()

    def z_final(prim, h, c2):
        step = steps[prim]
        src = w.at[2 * chip(step) + c2, rows(p)] if h == 0 else landed(prim, h, 1).at[c2]
        slot = 2 * chip(-step * h) + core
        return remote(
            src, wf.at[k, slot, rows(p)], fz_send, wz_recv.at[chip(-step * h)],
            {"z": chip(step), "core": c2},
        )

    def to_pair(zs, q):
        return remote(
            wf.at[k, pair(zs), rows(q)], wf.at[k, pair(zs), rows(q)], y_send, y_recv.at[zs], {"gl": 1 - p}
        )

    def x_move(d, slot, zs, q):
        return remote(
            wf.at[slot, pair(zs), rows(q)], wf.at[slot, pair(zs), rows(q)], x_send,
            x_recv.at[(1 - (q + d) % 2) * (1 + zs * n_gl + d)], {"tp": lax.rem(k + (1, n_tp - 1)[d], n_tp)},
        )

    def x_from(d):
        return lax.rem(k + (n_tp - 1, 1)[d], n_tp)

    def x_both(zs, q):
        x_move(0, k, zs, q).start()
        x_move(1, k, zs, q).start()

    def x_pass(d, slot, zs, q):
        return remote(
            wf.at[slot, pair(zs), rows(q)], wf.at[slot, pair(zs), rows(q)], r_send, x_recv.at[0],
            {"tp": lax.rem(k + (1, n_tp - 1)[d], n_tp)},
        )

    def relay(zs, q):
        if n_gl == 1:
            x_move(0, x_from(0), zs, q).wait_recv()
            x_pass(0, x_from(0), zs, q).start()
            return
        for d in range(2):

            @pl.when(q == d)
            def _():
                x_move(d, x_from(d), zs, d).wait_recv()
                x_pass(d, x_from(d), zs, d).start()

    def chips_at(level):
        if level == 0:
            return [z]
        if level == top:
            return [chip(top)]
        return [chip(-level), chip(level)]

    def arrive(level):
        for zs in chips_at(level):
            here = wf.at[k, pair(zs), rows(p)]
            remote(here, here, fz_send, wz_recv.at[zs], sibling).wait_recv()
            if n_gl == 2:
                to_pair(zs, p).start()
            x_both(zs, p)

    def other_half(level):
        if n_gl == 2:
            for zs in chips_at(level):
                to_pair(zs, 1 - p).wait_recv()
                x_both(zs, 1 - p)

    def forward(level, first, last):
        def one(j, carry):
            for prim in (True, False):

                @pl.when(j <= length[prim] - level)
                def _():
                    if level > 0:
                        z_wait(prim, level, j)
                    z_move(prim, level, j).start()

            return carry

        if first < last:
            lax.fori_loop(first, last, one, 0)

    def deliver(level):
        for prim in (True, False):
            if level < length[prim]:
                if level > 0:
                    z_wait(prim, level, 1)
                for c2 in range(2):
                    z_final(prim, level, c2).start()

    def part(ref, slot, q):
        return ref.at[slot, pl.ds(q * sub, sub)]

    def token(slot, q):
        return ct.at[slot] if q == 2 else part(xt, slot, q)

    def mine(q):
        return cq if q == 2 else xq.at[pl.ds(q * sub, sub)]

    t_recv = {True: tp_recv, False: ts_recv}

    def t_move(prim, h, q):
        step = steps[prim]
        slot = 2 * chip(-step * h) + core
        return remote(
            mine(q) if h == 0 else token(slot, q), token(slot, q), t_send.at[q // 2],
            t_recv[prim].at[h, q], {"z": chip(step)},
        )

    def t_wait(prim, h, q):
        here = token(2 * chip(-steps[prim] * h) + core, q)
        remote(here, here, t_send.at[q // 2], t_recv[prim].at[h - 1, q], sibling).wait_recv()

    def t_sibling(h, zs, q):
        slot = 2 * zs + core
        group = {0: 0, top - 1: 1}.get(h, 2)
        return remote(
            mine(q) if h == 0 else token(slot, q), token(slot, q), tb_send.at[q // 2], tb_recv.at[group, q // 2], sibling
        )

    def t_own(q):
        return pltpu.make_async_copy(mine(q), token(me, q), l_sem.at[1 + q])

    def tokens_out():
        for q in (2, 0, 1):
            for prim in (True, False):
                if length[prim] > 0:
                    t_move(prim, 0, q).start()
        for q in (2, 0, 1):
            t_sibling(0, z, q).start()
            t_own(q).start()

    def tokens_at(h):
        for q in (2, 0, 1):
            for prim in (True, False):
                if h <= length[prim]:
                    t_wait(prim, h, q)
                    if h < length[prim]:
                        t_move(prim, h, q).start()
                    t_sibling(h, chip(-steps[prim] * h), q).start()

    def own_block():
        return pltpu.make_async_copy(w.at[me], wf.at[k, me], l_sem.at[0])

    def sib_block(sender):
        return remote(w.at[2 * z + 1 - core], wf.at[k, sender], ws_send, ws_recv, sibling)

    relays = [(0, turn) for turn in range(n_gl)] + [
        (level, turn) for level in range(1, top + 1) for turn in range(n_gl)
    ]

    def pass_on(level, turn):
        while relays and relays[0] <= (level, turn):
            here, which = relays.pop(0)
            for zs in chips_at(here):
                relay(zs, which if here == 0 else lax.rem(p + which, n_gl))

    mixed_from = max(top - 2, 1)

    def weights_at(level):
        arrive(level)
        deliver(level)
        early = level <= mixed_from - 2
        if early and level > 1:
            pass_on(level - 1, 0)
        forward(level, 2, min(4, top - level + 1))
        if level <= mixed_from:
            other_half(level)
        if early:
            pass_on(level - 1, 1)
        forward(level, 4, top - level + 1)
        if level == mixed_from - 1:
            pass_on(level - 1, 0)
        if level == mixed_from:
            pass_on(level - 2, 1)

    after = {1: (top - 3, 0), 2: (top - 2, 0), 3: (top - 2, 1), 4: (top - 1, 1), 5: (top, 1)}
    due = list(range(mixed_from + 1, top + 1))

    def tokens_and_more(h, ready):
        tokens_at(h)
        if due and due[0] <= ready and h > 1:
            other_half(due.pop(0))
        if ready >= after.get(h, (top, 1))[0]:
            pass_on(*after.get(h, (-1, 0)))

    prepare(0)
    own_block().start()
    sib_block(me).start()
    deliver(0)
    forward(0, 2, 3)
    prepare(1)
    forward(0, 3, top + 1)
    own_block().wait()
    sib_block(me + 1 - 2 * core).wait_recv()
    for q in range(n_gl):
        x_both(z, q)
    prepare(2)
    h = 0
    for level in range(1, top + 1):
        if level == mixed_from:
            tokens_out()
        weights_at(level)
        if level >= mixed_from:
            h += 1
            tokens_and_more(h, level)

    def settle_weights():
        while due:
            other_half(due.pop(0))
        pass_on(top, 1)
        both = wf.at[pl.ds(0, 2)]
        remote(both, both, x_send, x_recv.at[0], sibling).wait_recv()
        for q in range(3):
            t_own(q).wait()

    def settle_tokens(group, count):
        for i, ref in enumerate((xt, ct)):
            here = ref.at[pl.ds(0, count)]
            remote(here, here, tb_send.at[i], tb_recv.at[group, i], sibling).wait_recv()

    started = h >= top
    for h in range(h + 1, top):
        tokens_and_more(h, top)
        if h == top - 2 and not relays and not due:
            settle_weights()
            settle_tokens(0, 1)
            first()
            started = True
    if not started or h >= top:
        settle_weights()
        settle_tokens(0, 1)
        first()
    settle_tokens(1, 2)
    second()
    if h < top:
        tokens_and_more(top, top)
    third()
    settle_tokens(2, n_z - 3)

    def drain():
        sib_block(me).wait_send()

        def sent(ref, sem):
            remote(ref, ref, sem, sem, sibling).wait_send()

        sent(wf.at[pl.ds(0, 2)], x_send)
        sent(wf.at[0], r_send)
        if n_gl == 2:
            sent(wf.at[0, pl.ds(0, n_z - 1)], y_send)
        sent(wf.at[0, pl.ds(0, 2 * (n_z - 1) // n_gl)], fz_send)
        sent(tbp, zp_send)
        if top > 2:
            sent(tbs, zs_send)
        for i, ref in enumerate((xt, ct)):
            sent(ref.at[pl.ds(0, n_z - 1)], t_send.at[i])
            sent(ref.at[pl.ds(0, n_z)], tb_send.at[i])

    return drain


def bring_scratch(n_z, n_tp, n_gl, w, xq, cq):
    top, n_fs = n_z // 2, 2 * n_z
    dma = pltpu.SemaphoreType.DMA
    prim, sec = top * (top + 1) // 2, top * (top - 1) // 2
    half = w[1] // n_gl
    return [
        pltpu.VMEM((n_tp, n_fs) + w[1:], bf16),
        pltpu.VMEM((n_fs,) + xq, bf16),
        pltpu.VMEM((n_fs,) + cq, f32),
        pltpu.VMEM((prim - top, 2, half, w[2]), bf16),
        pltpu.VMEM((max(sec - top + 1, 1), 2, half, w[2]), bf16),
        dma(()), dma((prim - top,)), dma(()), dma((max(sec - top + 1, 1),)),
        dma(()), dma((n_z,)), dma(()), dma((n_z,)), dma(()), dma((1 + n_z * n_gl,)), dma(()),
        dma((2,)), dma((top, 3)), dma((top - 1, 3)), dma((2,)), dma((3, 2)),
        dma((4,)), dma(()), dma(()),
    ]


def whole_kernel(
    n_z, n_tp, n_gl, n_bring, prompt, routes, weight, gain, gate, up, down,
    gate_out, up_out, down_out, mixed_out, w, xq, cq, g_in, u_in, d_in, in_sem, x_sem, out_sem, *scratch
):
    z, core, k, p = (lax.axis_index(a) for a in ("z", "core", "tp", "gl"))
    barrier = pltpu.get_barrier_semaphore()
    peers = [{"z": lax.rem(z + d, n_z), "core": c} for d in (1, n_z - 1) for c in range(2)]
    peers += [{"core": 1 - core}] + [{"tp": lax.rem(k + step, n_tp)} for step in range(1, n_tp)]
    if n_gl == 2:
        peers += [{"gl": 1 - p}]
    slots = g_in.shape[0]
    gate_rows, ffq = gate_out.shape[1:]
    share, cols = down_out.shape[0], w.shape[2]
    tok, width = xq.shape

    def fetch(n):
        off = ((n + 1) // 2) * (2 * (n % 2) - 1)
        rows = pl.ds(2 * lax.rem(z + off + n_z, n_z), 2)
        slot = lax.rem(n, slots)
        return [
            pltpu.make_async_copy(src.at[rows], dst.at[slot], in_sem.at[slot, i])
            for i, (src, dst) in enumerate(((gate, g_in), (up, u_in), (down, d_in)))
        ]

    def fetch_prompt():
        return pltpu.make_async_copy(prompt.at[pl.ds(pl.multiple_of(k * tok, tok), tok)], xq, x_sem)

    for n in range(slots):
        for copy in fetch(n):
            copy.start()
    fetch_prompt().start()
    for peer in peers:
        pl.semaphore_signal(barrier, inc=1, device_id=peer, device_id_type=MESH)
    square = lax.broadcasted_iota(jnp.int32, (gate_rows, gate_rows), 0) == lax.broadcasted_iota(
        jnp.int32, (gate_rows, gate_rows), 1
    )
    column = jnp.sum(jnp.where(square, gain[...], 0.0), axis=1, keepdims=True)

    def convert(n, carry):
        off = ((n + 1) // 2) * (2 * (n % 2) - 1)
        first = 2 * lax.rem(z + off + n_z, n_z)
        slot = lax.rem(n, slots)
        for copy in fetch(n):
            copy.wait()
        for e in range(2):
            w[first + e, :gate_rows, :ffq] = (column * g_in[slot, e]).astype(bf16)
            w[first + e, :gate_rows, ffq:] = (column * u_in[slot, e]).astype(bf16)
            w[first + e, gate_rows:, :] = d_in[slot, e].astype(bf16)

        @pl.when(n + slots < n_z)
        def _():
            for copy in fetch(n + slots):
                copy.start()

        return carry

    def normalize(r, carry):
        rows = pl.ds(pl.multiple_of(r * 16, 16), 16)
        v = xq[rows, :].astype(f32)
        xq[rows, :] = (v * lax.rsqrt(jnp.mean(v * v, axis=-1, keepdims=True) + EPS)).astype(bf16)
        return carry

    def part_of(ref):
        mine = ref[:, :tok]
        for t in range(1, n_tp):
            mine = jnp.where(k == t, ref[:, t * tok : (t + 1) * tok], mine)
        return mine

    def prepare(stage):
        early = min(5, n_z)
        if stage == 0:
            lax.fori_loop(0, early, convert, 0)
            pl.semaphore_wait(barrier, len(peers))
        if stage == 1:
            lax.fori_loop(early, n_z, convert, 0)
        if stage == 2:
            fetch_prompt().wait()
            lax.fori_loop(0, tok // 16, normalize, 0)
            chosen, amount = part_of(routes), part_of(weight)
            index = lax.broadcasted_iota(jnp.int32, (cq.shape[0], tok), 0)
            total = jnp.zeros((cq.shape[0], tok), f32)
            for j in range(chosen.shape[0]):
                total += jnp.where(index == chosen[j : j + 1, :], amount[j : j + 1, :], 0.0)
            cq[...] = jnp.zeros_like(cq)
            cq[:, :tok] = total

    for_bring, for_apply = scratch[:n_bring], scratch[n_bring:]
    wf, xt, ct = for_bring[:3]
    outs = [
        pltpu.make_async_copy(wf.at[k, :, :gate_rows, :ffq], gate_out, out_sem.at[0]),
        pltpu.make_async_copy(wf.at[k, :, :gate_rows, ffq:], up_out, out_sem.at[1]),
    ]
    for t in range(n_tp):
        outs.append(
            pltpu.make_async_copy(
                wf.at[t, pl.ds(k * share, share), gate_rows:, :],
                down_out.at[:, :, t * cols : (t + 1) * cols],
                out_sem.at[2 + t],
            )
        )
    first, second, third, rest = apply_and_return(n_z, n_tp, wf, xt, ct, mixed_out, *for_apply)

    def weights_ready():
        for copy in outs:
            copy.start()
        first()

    drain = bring(n_z, n_tp, n_gl, prepare, weights_ready, second, third, w, xq, cq, *for_bring)

    def finish():
        for copy in outs:
            copy.wait()
        drain()

    rest(finish)


def hand_over(*refs):
    n = (len(refs) - 2) // 3
    srcs, outs, bufs = refs[:n], refs[n : 2 * n], refs[2 * n : 3 * n]
    in_sem, out_sem = refs[3 * n :]
    reads, writes = [], []
    for i, (src, out, buf) in enumerate(zip(srcs, outs, bufs)):
        half = src.shape[0] // 2
        for j in range(2):
            rows = pl.ds(j * half, half)
            reads.append(pltpu.make_async_copy(src.at[rows], buf.at[rows], in_sem.at[i, j]))
            writes.append(pltpu.make_async_copy(buf.at[rows], out.at[rows], out_sem.at[i, j]))
    for copy in reads:
        copy.start()
    for read, write in zip(reads, writes):
        read.wait()
        write.start()
    for copy in writes:
        copy.wait()


def shards(prompt, routes, route_weight, norm_gain, gate_train, up_train, down_train):
    n_tp, n_z, n_gl = lax.axis_size("tp"), lax.axis_size("z"), lax.axis_size("gl")
    n_fs = 2 * n_z
    experts, gate_rows, ffq = gate_train.shape
    down_rows, cols = down_train.shape[1:]
    tok, d = prompt.shape[0] // n_tp, prompt.shape[1]
    lanes = -(-tok // 128) * 128
    share = n_fs // n_tp
    slots = 3
    w_shape = (experts, gate_rows + down_rows, cols)
    x_shape, c_shape = (tok, d), (experts, lanes)
    vmem = pl.BlockSpec(memory_space=pltpu.VMEM)
    hbm = pl.BlockSpec(memory_space=pl.ANY)
    for_bring = bring_scratch(n_z, n_tp, n_gl, w_shape, x_shape, c_shape)
    dma = pltpu.SemaphoreType.DMA
    gate_own, up_own, down_own, mixed = pl.pallas_call(
        functools.partial(whole_kernel, n_z, n_tp, n_gl, len(for_bring)),
        out_shape=(
            jax.ShapeDtypeStruct((n_fs, gate_rows, ffq), bf16),
            jax.ShapeDtypeStruct((n_fs, gate_rows, ffq), bf16),
            jax.ShapeDtypeStruct((share, down_rows, n_tp * cols), bf16),
            jax.ShapeDtypeStruct((tok * n_tp, cols), bf16),
        ),
        in_specs=[hbm] + [vmem] * 3 + [hbm] * 3,
        out_specs=(hbm, hbm, hbm, vmem),
        scratch_shapes=[
            pltpu.VMEM(w_shape, bf16),
            pltpu.VMEM(x_shape, bf16),
            pltpu.VMEM(c_shape, f32),
            pltpu.VMEM((slots, 2, gate_rows, ffq), f32),
            pltpu.VMEM((slots, 2, gate_rows, ffq), f32),
            pltpu.VMEM((slots, 2, down_rows, cols), f32),
            dma((slots, 3)),
            dma(()),
            dma((2 + n_tp,)),
        ]
        + for_bring
        + apply_scratch(n_z, n_tp, n_fs, tok, d),
        compiler_params=pltpu.CompilerParams(
            collective_id=0, has_side_effects=True, vmem_limit_bytes=67043328
        ),
    )(prompt, routes.T, route_weight.T, norm_gain[None, :], gate_train, up_train, down_train)
    results = (gate_own, up_own, down_own, mixed)
    gate_own, up_own, down_own, mixed = pl.pallas_call(
        hand_over,
        out_shape=tuple(jax.ShapeDtypeStruct(a.shape, a.dtype) for a in results),
        in_specs=[hbm] * 4,
        out_specs=[hbm] * 4,
        scratch_shapes=[pltpu.VMEM(a.shape, a.dtype) for a in results] + [dma((4, 2)), dma((4, 2))],
        compiler_params=pltpu.CompilerParams(vmem_limit_bytes=67043328),
    )(*results)
    return (
        gate_own.reshape(1, d, ffq),
        up_own.reshape(1, d, ffq),
        down_own.reshape(1, share * down_rows, n_tp * cols),
        mixed,
    )


def solution(mesh):
    groups, n_tp = mesh.shape["grp"], mesh.shape["tp"]
    chips = mesh.shape["fs"] // 2
    pair = 2 if groups % 2 == 0 else 1
    finer = Mesh(
        mesh.devices.reshape(groups // pair, pair, chips, 2, n_tp),
        ("gh", "gl", "z", "core", "tp"),
    )
    return jax.shard_map(
        shards,
        mesh=finer,
        in_specs=(P(ROWS), P(ROWS), P(ROWS), P(FS), P(None, FS, "tp"), P(None, FS, "tp"), P(None, FS, "tp")),
        out_specs=(P(ROWS, None, "tp"), P(ROWS, None, "tp"), P(ROWS, "tp", None), P(ROWS, "tp")),
        check_vma=False,
    )
```

```python
import functools

import jax
import jax.numpy as jnp
from jax import lax
from jax.experimental import pallas as pl
from jax.experimental.pallas import tpu as pltpu
from jax.sharding import Mesh
from jax.sharding import PartitionSpec as P

LIMIT = 7.0
ALPHA = 1.702
EPS = 1e-06
FS = ("z", "core")
ROWS = ("gh", "gl", "z", "core")
MESH = pl.DeviceIdType.MESH
f32, bf16 = jnp.float32, jnp.bfloat16


def remote(src, dst, send, recv, where):
    return pltpu.make_async_remote_copy(
        src_ref=src, dst_ref=dst, send_sem=send, recv_sem=recv, device_id=where, device_id_type=MESH
    )


def apply_and_return(
    n_z, n_tp, wf, xt, ct, out, hid, cb, sib, acc_p, acc_s, fin,
    p_send, p_recv, s_send, s_recv, b_send, b_recv, f_send, f_recv,
):
    z, core, k = lax.axis_index("z"), lax.axis_index("core"), lax.axis_index("tp")
    steps = n_z // 2
    tok, width = xt.shape[1], xt.shape[2]
    sub = tok // 2
    cols = width // n_tp
    ffq = cols // 2
    gate_rows = width // wf.shape[1]
    down_rows = wf.shape[2] - gate_rows
    sign = 1 - 2 * core
    ahead = lax.rem(z + sign + n_z, n_z)
    behind = lax.rem(z - sign + n_z, n_z)
    sibling = {"core": 1 - core}

    def chips(i):
        j = steps - i
        return lax.rem(z + j, n_z), lax.rem(z - j + n_z, n_z)

    def span(q):
        return (0, tok) if q is None else (q * sub, sub)

    def inner(some, q=None):
        at, count = span(q)
        x = jnp.concatenate([xt[2 * chip + c, at : at + count, :] for chip in some for c in range(2)], axis=0)
        count = x.shape[0]
        for t in range(n_tp):
            gu = jnp.dot(x, wf[t, :, :gate_rows, :].reshape(width, cols), preferred_element_type=f32)
            g = jnp.minimum(gu[:, :ffq], LIMIT)
            u = jnp.clip(gu[:, ffq:], -LIMIT, LIMIT)
            hid[:count, t * ffq : (t + 1) * ffq] = ((u + 1.0) * g * jax.nn.sigmoid(ALPHA * g)).astype(bf16)

    def outer(some, places, q=None):
        at, count = span(q)
        total = 2 * count * len(some)
        eye = lax.broadcasted_iota(jnp.int32, (tok, ct.shape[2]), 0) == lax.broadcasted_iota(
            jnp.int32, (tok, ct.shape[2]), 1
        )
        own = lax.broadcasted_iota(jnp.int32, ct.shape[1:], 0) == 2 * z + core
        scales = []
        for chip in some:
            for c in range(2):
                row = jnp.sum(jnp.where(own, ct[2 * chip + c].astype(f32), 0.0), axis=0, keepdims=True)
                scales.append(jnp.sum(jnp.where(eye, row, 0.0), axis=1, keepdims=True)[at : at + count])
        scale = jnp.concatenate(scales, axis=0)
        for t in range(n_tp):
            down = wf[t, :, gate_rows:, :].reshape(wf.shape[1] * down_rows, cols)
            part = (scale * jnp.dot(hid[:total, :], down, preferred_element_type=f32)).astype(bf16)
            for n, (i, w) in enumerate(places):
                for c in range(2):
                    here = (2 * n + c) * count
                    cb[i, w, c, at : at + count, t * cols : (t + 1) * cols] = part[here : here + count]

    def b_slot(i, w):
        return steps * w if isinstance(i, int) and i == 0 else i

    def to_sibling(i, w):
        return remote(cb.at[i, w, 1 - core], sib.at[i, w], b_send, b_recv.at[b_slot(i, w)], sibling)

    def hop_p(h, q):
        rows = pl.ds(q * sub, sub)
        return remote(
            acc_p.at[h, rows], acc_p.at[h + 1, rows], p_send, p_recv.at[h, q], {"z": ahead}
        )

    def hop_s(h, q):
        rows = pl.ds(q * sub, sub)
        return remote(
            acc_s.at[h, rows], acc_s.at[h + 1, rows], s_send, s_recv.at[h - 1, q], {"z": behind}
        )

    def local(h, w, rows):
        return cb[h, w, core, rows, :].astype(f32) + sib[h, w, rows, :].astype(f32)

    def combine_p(h, q):
        rows = pl.ds(q * sub, sub)
        prim = jnp.where(h == 0, 0, core)

        @pl.when(h == 0)
        def _():
            acc_p[h, rows, :] = local(h, prim, rows).astype(bf16)

        @pl.when(h > 0)
        def _():
            hop_p(h - 1, q).wait_recv()
            acc_p[h, rows, :] = (local(h, prim, rows) + acc_p[h, rows, :].astype(f32)).astype(bf16)

        hop_p(h, q).start()

    def combine_s(h, q):
        rows = pl.ds(q * sub, sub)

        @pl.when(h == 1)
        def _():
            acc_s[h, rows, :] = local(h, 1 - core, rows).astype(bf16)

        @pl.when(h > 1)
        def _():
            hop_s(h - 1, q).wait_recv()
            acc_s[h, rows, :] = (local(h, 1 - core, rows) + acc_s[h, rows, :].astype(f32)).astype(bf16)

        hop_s(h, q).start()

    def sib_in(i):
        remote(sib.at[i], sib.at[i], b_send, b_recv.at[i], sibling).wait_recv()

    def sib_out(i):
        for w in range(2):
            to_sibling(i, w).start()

    def begin(i):
        @pl.when(i > 1)
        def _():
            sib_in(i)
            combine_s(i, 0)

        @pl.when(i == 1)
        def _():
            to_sibling(0, 0).wait_recv()

        combine_p(i - 1, 0)

        @pl.when(i == 1)
        def _():
            combine_p(i - 1, 1)

    def end(i):
        @pl.when(i > 1)
        def _():
            combine_s(i, 1)
            combine_p(i - 1, 1)

    def body(i, carry):
        begin(i)
        inner(chips(i + 2))
        end(i)
        outer(chips(i + 2), [(i + 2, 0), (i + 2, 1)])
        sib_out(i + 2)
        return carry

    def ahead_of_near():
        inner(chips(2))
        outer(chips(2), [(2, 0), (2, 1)])
        sib_out(2)

    def one_chip(chip, w):
        inner([chip])
        outer([chip], [(0, w)])
        to_sibling(0, w).start()

    def to_tp(t, q):
        rows = pl.ds(q * sub, sub)
        at = pl.multiple_of(k * tok + q * sub, sub)
        return remote(fin.at[t, rows], out.at[pl.ds(at, sub)], f_send, f_recv, {"tp": t})

    def sent(ref, sem):
        remote(ref, ref, sem, sem, sibling).wait_send()

    def first():
        one_chip(z, 1)

    def near_sibling(w, q):
        rows = pl.ds(q * sub, sub)
        return remote(
            cb.at[1, w, 1 - core, rows], sib.at[1, w, rows], b_send, b_recv.at[1 + q * steps], sibling
        )

    def second(q):
        inner(chips(1), q)
        outer(chips(1), [(1, 0), (1, 1)], q)
        for w in range(2):
            near_sibling(w, q).start()

    def third(q):
        here = sib.at[1, :, pl.ds(q * sub, sub)]
        remote(here, here, b_send, b_recv.at[1 + q * steps], sibling).wait_recv()
        combine_s(1, q)

    def rest(drain_bring):
        one_chip(lax.rem(z + steps, n_z), 0)
        lax.fori_loop(1, max(steps - 2, 1), body, 0)
        last = steps - 1
        if last > 1:
            begin(last - 1)
            end(last - 1)
        if last == 1:
            to_sibling(0, 0).wait_recv()
        else:
            sib_in(last)
        for q in range(2):
            if last > 1:
                combine_s(last, q)
            combine_p(last - 1, q)
        for q in range(2):
            combine_p(last, q)
        to_sibling(0, 1).wait_recv()
        drain_bring()
        sent(sib, b_send)
        for q in range(2):
            rows = pl.ds(q * sub, sub)
            hop_p(steps - 1, q).wait_recv()
            hop_s(steps - 1, q).wait_recv()
            total = (
                local(0, 1, rows)
                + acc_p[steps, rows, :].astype(f32)
                + acc_s[steps, rows, :].astype(f32)
            ).astype(bf16)
            for t in range(n_tp):
                fin[t, rows, :] = total[:, t * cols : (t + 1) * cols]
            for step in (2, 1, 3):
                to_tp(lax.rem(k + step, n_tp), q).start()
            out[pl.ds(pl.multiple_of(k * tok + q * sub, sub), sub), :] = fin[k, rows, :]
        sent(acc_p.at[pl.ds(0, steps)], p_send)
        sent(acc_s.at[pl.ds(0, steps - 1)], s_send)
        peers = fin.at[pl.ds(0, n_tp - 1)]
        sent(peers, f_send)
        remote(peers, peers, f_send, f_recv, sibling).wait_recv()

    return first, ahead_of_near, second, third, rest


def apply_scratch(n_z, n_tp, n_fs, tok, width):
    steps = n_z // 2
    dma = pltpu.SemaphoreType.DMA
    return [
        pltpu.VMEM((4 * tok, width // 2), bf16),
        pltpu.VMEM((steps, 2, 2, tok, width), bf16),
        pltpu.VMEM((steps, 2, tok, width), bf16),
        pltpu.VMEM((steps + 1, tok, width), bf16),
        pltpu.VMEM((steps + 1, tok, width), bf16),
        pltpu.VMEM((n_tp, tok, width // n_tp), bf16),
        dma(()), dma((steps, 2)), dma(()), dma((steps - 1, 2)), dma(()), dma((steps + 2,)), dma(()), dma(()),
    ]


def bring(
    n_z, n_tp, n_gl, prepare, first, ahead_of_near, second, third, w, xq, cq, wf, xt, ct, tbp, tbs,
    zp_send, zp_recv, zs_send, zs_recv, fz_send, wz_recv, y_send, y_recv, x_send, x_recv, r_send,
    t_send, tp_recv, ts_recv, tb_send, tb_recv, l_sem, ws_send, ws_recv,
):
    z, core, k, p = (lax.axis_index(a) for a in ("z", "core", "tp", "gl"))
    top = n_z // 2
    me = 2 * z + core
    sign = 1 - 2 * core
    half = w.shape[1] // n_gl
    sub = xq.shape[0] // 2
    steps = {True: sign, False: -sign}
    length = {True: top, False: top - 1}
    transit = {True: tbp, False: tbs}
    z_send = {True: zp_send, False: zs_send}
    z_recv = {True: zp_recv, False: zs_recv}
    sibling = {"core": 1 - core}

    def chip(v):
        return lax.rem(z + v + 2 * n_z, n_z)

    def rows(q):
        return pl.ds(pl.multiple_of(q * half, half), half)

    def pair(zs):
        return pl.ds(2 * zs, 2)

    def tri(prim, h, j):
        return h * length[prim] - h * (h - 1) // 2 + j - 1

    def landed(prim, h, j):
        return transit[prim].at[tri(prim, h, j) - length[prim]]

    def z_move(prim, h, j):
        step = steps[prim]
        src = w.at[pair(chip(step * j)), rows(p)] if h == 0 else landed(prim, h, j)
        return remote(
            src, landed(prim, h + 1, j - 1), z_send[prim],
            z_recv[prim].at[tri(prim, h + 1, j - 1) - length[prim]], {"z": chip(step)},
        )

    def z_wait(prim, h, j):
        here = landed(prim, h, j)
        at = tri(prim, h, j) - length[prim]
        remote(here, here, z_send[prim], z_recv[prim].at[at], {"z": chip(steps[prim])}).wait_recv()

    def z_final(prim, h, c2):
        step = steps[prim]
        src = w.at[2 * chip(step) + c2, rows(p)] if h == 0 else landed(prim, h, 1).at[c2]
        slot = 2 * chip(-step * h) + core
        return remote(
            src, wf.at[k, slot, rows(p)], fz_send, wz_recv.at[chip(-step * h)],
            {"z": chip(step), "core": c2},
        )

    def to_pair(zs, q):
        return remote(
            wf.at[k, pair(zs), rows(q)], wf.at[k, pair(zs), rows(q)], y_send, y_recv.at[zs], {"gl": 1 - p}
        )

    def x_move(d, slot, zs, q):
        return remote(
            wf.at[slot, pair(zs), rows(q)], wf.at[slot, pair(zs), rows(q)], x_send,
            x_recv.at[(1 - (q + d) % 2) * (1 + zs * n_gl + d)], {"tp": lax.rem(k + (1, n_tp - 1)[d], n_tp)},
        )

    def x_from(d):
        return lax.rem(k + (n_tp - 1, 1)[d], n_tp)

    def x_both(zs, q):
        x_move(0, k, zs, q).start()
        x_move(1, k, zs, q).start()

    def x_pass(d, slot, zs, q):
        return remote(
            wf.at[slot, pair(zs), rows(q)], wf.at[slot, pair(zs), rows(q)], r_send, x_recv.at[0],
            {"tp": lax.rem(k + (1, n_tp - 1)[d], n_tp)},
        )

    def relay(zs, q):
        if n_gl == 1:
            x_move(0, x_from(0), zs, q).wait_recv()
            x_pass(0, x_from(0), zs, q).start()
            return
        for d in range(2):

            @pl.when(q == d)
            def _():
                x_move(d, x_from(d), zs, d).wait_recv()
                x_pass(d, x_from(d), zs, d).start()

    def chips_at(level):
        if level == 0:
            return [z]
        if level == top:
            return [chip(top)]
        return [chip(-level), chip(level)]

    def arrive(level):
        for zs in chips_at(level):
            here = wf.at[k, pair(zs), rows(p)]
            remote(here, here, fz_send, wz_recv.at[zs], sibling).wait_recv()
            if n_gl == 2:
                to_pair(zs, p).start()
            x_both(zs, p)

    def other_half(level):
        if n_gl == 2:
            for zs in chips_at(level):
                to_pair(zs, 1 - p).wait_recv()
                x_both(zs, 1 - p)

    def forward(level, first, last):
        def one(j, carry):
            for prim in (True, False):

                @pl.when(j <= length[prim] - level)
                def _():
                    if level > 0:
                        z_wait(prim, level, j)
                    z_move(prim, level, j).start()

            return carry

        if first < last:
            lax.fori_loop(first, last, one, 0)

    def deliver(level):
        for prim in (True, False):
            if level < length[prim]:
                if level > 0:
                    z_wait(prim, level, 1)
                for c2 in range(2):
                    z_final(prim, level, c2).start()

    def part(ref, slot, q):
        return ref.at[slot, pl.ds(q * sub, sub)]

    def token(slot, q):
        return ct.at[slot] if q == 2 else part(xt, slot, q)

    def mine(q):
        return cq if q == 2 else xq.at[pl.ds(q * sub, sub)]

    t_recv = {True: tp_recv, False: ts_recv}

    def t_move(prim, h, q):
        step = steps[prim]
        slot = 2 * chip(-step * h) + core
        return remote(
            mine(q) if h == 0 else token(slot, q), token(slot, q), t_send.at[q // 2],
            t_recv[prim].at[h, q], {"z": chip(step)},
        )

    def t_wait(prim, h, q):
        here = token(2 * chip(-steps[prim] * h) + core, q)
        remote(here, here, t_send.at[q // 2], t_recv[prim].at[h - 1, q], sibling).wait_recv()

    def t_sibling(h, zs, q):
        slot = 2 * zs + core
        group = 0 if h == 0 else 4 if h == top - 2 else 3 if h != top - 1 else 2 if q == 1 else 1
        return remote(
            mine(q) if h == 0 else token(slot, q), token(slot, q), tb_send.at[q // 2], tb_recv.at[group, q // 2], sibling
        )

    def t_own(q):
        return pltpu.make_async_copy(mine(q), token(me, q), l_sem.at[1 + q])

    def tokens_out():
        for q in (2, 0, 1):
            for prim in (True, False):
                if length[prim] > 0:
                    t_move(prim, 0, q).start()
        for q in (2, 0, 1):
            t_sibling(0, z, q).start()
            t_own(q).start()

    def tokens_at(h, parts=(2, 0, 1)):
        for q in parts:
            for prim in (True, False):
                if h <= length[prim]:
                    t_wait(prim, h, q)
                    if h < length[prim]:
                        t_move(prim, h, q).start()
                    t_sibling(h, chip(-steps[prim] * h), q).start()

    def own_block():
        return pltpu.make_async_copy(w.at[me], wf.at[k, me], l_sem.at[0])

    def sib_block(sender):
        return remote(w.at[2 * z + 1 - core], wf.at[k, sender], ws_send, ws_recv, sibling)

    relays = [(0, turn) for turn in range(n_gl)] + [
        (level, turn) for level in range(1, top + 1) for turn in range(n_gl)
    ]

    def pass_on(level, turn):
        while relays and relays[0] <= (level, turn):
            here, which = relays.pop(0)
            for zs in chips_at(here):
                relay(zs, which if here == 0 else lax.rem(p + which, n_gl))

    mixed_from = max(top - 2, 1)

    def weights_at(level):
        arrive(level)
        deliver(level)
        early = level <= mixed_from - 2
        if early and level > 1:
            pass_on(level - 1, 0)
        forward(level, 2, min(4, top - level + 1))
        if level <= mixed_from:
            other_half(level)
        if early:
            pass_on(level - 1, 1)
        forward(level, 4, top - level + 1)
        if level == mixed_from - 1:
            pass_on(level - 1, 0)
        if level == mixed_from:
            pass_on(level - 2, 1)

    after = {1: (top - 3, 0), 2: (top - 2, 0), 3: (top - 2, 1), 4: (top - 1, 1), 5: (top, 1)}
    due = list(range(mixed_from + 1, top + 1))

    def tokens_and_more(h, ready):
        tokens_at(h)
        if due and due[0] <= ready and h > 1:
            other_half(due.pop(0))
        if ready >= after.get(h, (top, 1))[0]:
            pass_on(*after.get(h, (-1, 0)))

    prepare(0)
    own_block().start()
    sib_block(me).start()
    deliver(0)
    forward(0, 2, 3)
    prepare(1)
    forward(0, 3, top + 1)
    own_block().wait()
    sib_block(me + 1 - 2 * core).wait_recv()
    for q in range(n_gl):
        x_both(z, q)
    prepare(2)
    h = 0
    for level in range(1, top + 1):
        if level == mixed_from:
            tokens_out()
        weights_at(level)
        if level >= mixed_from:
            h += 1
            tokens_and_more(h, level)

    def settle_weights():
        while due:
            other_half(due.pop(0))
        pass_on(top, 1)
        both = wf.at[pl.ds(0, 2)]
        remote(both, both, x_send, x_recv.at[0], sibling).wait_recv()
        for q in range(3):
            t_own(q).wait()

    def settle_tokens(group, *refs):
        for i, here in enumerate(refs):
            remote(here, here, tb_send.at[i], tb_recv.at[group, i], sibling).wait_recv()

    def own_tokens():
        settle_weights()
        settle_tokens(0, xt.at[pl.ds(0, 1)], ct.at[pl.ds(0, 1)])
        first()

    def near_tokens(q):
        here = xt.at[pl.ds(0, 2), pl.ds(0, sub)]
        settle_tokens(1 + q, *((here, ct.at[pl.ds(0, 2)])[: 2 - q]))
        second(q)

    started = False
    while h + 1 < top - 1:
        h += 1
        tokens_and_more(h, top)
        if h == top - 2 and not relays and not due:
            own_tokens()
            started = True
    if not started:
        own_tokens()
    if h < top - 1:
        tokens_at(top - 1, (2, 0))
    if top > 2:
        settle_tokens(4, xt.at[pl.ds(0, 2)], ct.at[pl.ds(0, 2)])
        ahead_of_near()
    if h < top - 1:
        tokens_at(top - 1, (1,))
    if h < top:
        tokens_at(top, (2, 0))
    near_tokens(0)
    near_tokens(1)
    third(0)
    if h < top:
        tokens_at(top, (1,))
    third(1)
    rest = pl.ds(0, n_z - (5 if top > 2 else 3))
    settle_tokens(3, xt.at[rest], ct.at[rest])

    def drain():
        sib_block(me).wait_send()

        def sent(ref, sem):
            remote(ref, ref, sem, sem, sibling).wait_send()

        sent(wf.at[pl.ds(0, 2)], x_send)
        sent(wf.at[0], r_send)
        if n_gl == 2:
            sent(wf.at[0, pl.ds(0, n_z - 1)], y_send)
        sent(wf.at[0, pl.ds(0, 2 * (n_z - 1) // n_gl)], fz_send)
        sent(tbp, zp_send)
        if top > 2:
            sent(tbs, zs_send)
        for i, ref in enumerate((xt, ct)):
            sent(ref.at[pl.ds(0, n_z - 1)], t_send.at[i])
            sent(ref.at[pl.ds(0, n_z)], tb_send.at[i])

    return drain


def bring_scratch(n_z, n_tp, n_gl, w, xq, cq):
    top, n_fs = n_z // 2, 2 * n_z
    dma = pltpu.SemaphoreType.DMA
    prim, sec = top * (top + 1) // 2, top * (top - 1) // 2
    half = w[1] // n_gl
    return [
        pltpu.VMEM((n_tp, n_fs) + w[1:], bf16),
        pltpu.VMEM((n_fs,) + xq, bf16),
        pltpu.VMEM((n_fs,) + cq, bf16),
        pltpu.VMEM((prim - top, 2, half, w[2]), bf16),
        pltpu.VMEM((max(sec - top + 1, 1), 2, half, w[2]), bf16),
        dma(()), dma((prim - top,)), dma(()), dma((max(sec - top + 1, 1),)),
        dma(()), dma((n_z,)), dma(()), dma((n_z,)), dma(()), dma((1 + n_z * n_gl,)), dma(()),
        dma((2,)), dma((top, 3)), dma((top - 1, 3)), dma((2,)), dma((5, 2)),
        dma((4,)), dma(()), dma(()),
    ]


def whole_kernel(
    n_z, n_tp, n_gl, n_bring, prompt, routes, weight, gain, gate, up, down,
    gate_out, up_out, down_out, mixed_out, w, xq, cq, g_in, u_in, d_in, in_sem, x_sem, out_sem, *scratch
):
    z, core, k, p = (lax.axis_index(a) for a in ("z", "core", "tp", "gl"))
    barrier = pltpu.get_barrier_semaphore()
    peers = [{"z": lax.rem(z + d, n_z), "core": c} for d in (1, n_z - 1) for c in range(2)]
    peers += [{"core": 1 - core}] + [{"tp": lax.rem(k + step, n_tp)} for step in range(1, n_tp)]
    if n_gl == 2:
        peers += [{"gl": 1 - p}]
    slots = g_in.shape[0]
    gate_rows, ffq = gate_out.shape[1:]
    share, cols = down_out.shape[0], w.shape[2]
    tok, width = xq.shape

    def fetch(n):
        off = ((n + 1) // 2) * (2 * (n % 2) - 1)
        rows = pl.ds(2 * lax.rem(z + off + n_z, n_z), 2)
        slot = lax.rem(n, slots)
        return [
            pltpu.make_async_copy(src.at[rows], dst.at[slot], in_sem.at[slot, i])
            for i, (src, dst) in enumerate(((gate, g_in), (up, u_in), (down, d_in)))
        ]

    def fetch_prompt():
        return pltpu.make_async_copy(prompt.at[pl.ds(pl.multiple_of(k * tok, tok), tok)], xq, x_sem)

    for n in range(slots):
        for copy in fetch(n):
            copy.start()
    fetch_prompt().start()
    for peer in peers:
        pl.semaphore_signal(barrier, inc=1, device_id=peer, device_id_type=MESH)
    square = lax.broadcasted_iota(jnp.int32, (gate_rows, gate_rows), 0) == lax.broadcasted_iota(
        jnp.int32, (gate_rows, gate_rows), 1
    )
    column = jnp.sum(jnp.where(square, gain[...], 0.0), axis=1, keepdims=True)

    def convert(n, carry):
        off = ((n + 1) // 2) * (2 * (n % 2) - 1)
        first = 2 * lax.rem(z + off + n_z, n_z)
        slot = lax.rem(n, slots)
        for copy in fetch(n):
            copy.wait()
        for e in range(2):
            w[first + e, :gate_rows, :ffq] = (column * g_in[slot, e]).astype(bf16)
            w[first + e, :gate_rows, ffq:] = (column * u_in[slot, e]).astype(bf16)
            w[first + e, gate_rows:, :] = d_in[slot, e].astype(bf16)

        @pl.when(n + slots < n_z)
        def _():
            for copy in fetch(n + slots):
                copy.start()

        return carry

    def normalize(r, carry):
        rows = pl.ds(pl.multiple_of(r * 16, 16), 16)
        v = xq[rows, :].astype(f32)
        xq[rows, :] = (v * lax.rsqrt(jnp.mean(v * v, axis=-1, keepdims=True) + EPS)).astype(bf16)
        return carry

    def part_of(ref):
        mine = ref[:, :tok]
        for t in range(1, n_tp):
            mine = jnp.where(k == t, ref[:, t * tok : (t + 1) * tok], mine)
        return mine

    def prepare(stage):
        early = min(5, n_z)
        if stage == 0:
            lax.fori_loop(0, early, convert, 0)
            pl.semaphore_wait(barrier, len(peers))
        if stage == 1:
            lax.fori_loop(early, n_z, convert, 0)
        if stage == 2:
            fetch_prompt().wait()
            lax.fori_loop(0, tok // 16, normalize, 0)
            chosen, amount = part_of(routes), part_of(weight)
            index = lax.broadcasted_iota(jnp.int32, (cq.shape[0], tok), 0)
            total = jnp.zeros((cq.shape[0], tok), f32)
            for j in range(chosen.shape[0]):
                total += jnp.where(index == chosen[j : j + 1, :], amount[j : j + 1, :], 0.0)
            cq[...] = jnp.zeros_like(cq)
            cq[:, :tok] = total.astype(bf16)

    for_bring, for_apply = scratch[:n_bring], scratch[n_bring:]
    wf, xt, ct = for_bring[:3]
    outs = [
        pltpu.make_async_copy(wf.at[k, :, :gate_rows, :ffq], gate_out, out_sem.at[0]),
        pltpu.make_async_copy(wf.at[k, :, :gate_rows, ffq:], up_out, out_sem.at[1]),
    ]
    for t in range(n_tp):
        outs.append(
            pltpu.make_async_copy(
                wf.at[t, pl.ds(k * share, share), gate_rows:, :],
                down_out.at[:, :, t * cols : (t + 1) * cols],
                out_sem.at[2 + t],
            )
        )
    first, ahead_of_near, second, third, rest = apply_and_return(n_z, n_tp, wf, xt, ct, mixed_out, *for_apply)

    def weights_ready():
        for copy in outs:
            copy.start()
        first()

    drain = bring(n_z, n_tp, n_gl, prepare, weights_ready, ahead_of_near, second, third, w, xq, cq, *for_bring)

    def finish():
        for copy in outs:
            copy.wait()
        drain()

    rest(finish)


def hand_over(*refs):
    n = (len(refs) - 2) // 3
    srcs, outs, bufs = refs[:n], refs[n : 2 * n], refs[2 * n : 3 * n]
    in_sem, out_sem = refs[3 * n :]
    reads, writes = [], []
    for i, (src, out, buf) in enumerate(zip(srcs, outs, bufs)):
        half = src.shape[0] // 2
        for j in range(2):
            rows = pl.ds(j * half, half)
            reads.append(pltpu.make_async_copy(src.at[rows], buf.at[rows], in_sem.at[i, j]))
            writes.append(pltpu.make_async_copy(buf.at[rows], out.at[rows], out_sem.at[i, j]))
    for copy in reads:
        copy.start()
    for read, write in zip(reads, writes):
        read.wait()
        write.start()
    for copy in writes:
        copy.wait()


def shards(prompt, routes, route_weight, norm_gain, gate_train, up_train, down_train):
    n_tp, n_z, n_gl = lax.axis_size("tp"), lax.axis_size("z"), lax.axis_size("gl")
    n_fs = 2 * n_z
    experts, gate_rows, ffq = gate_train.shape
    down_rows, cols = down_train.shape[1:]
    tok, d = prompt.shape[0] // n_tp, prompt.shape[1]
    lanes = -(-tok // 128) * 128
    share = n_fs // n_tp
    slots = 3
    w_shape = (experts, gate_rows + down_rows, cols)
    x_shape, c_shape = (tok, d), (experts, lanes)
    vmem = pl.BlockSpec(memory_space=pltpu.VMEM)
    hbm = pl.BlockSpec(memory_space=pl.ANY)
    for_bring = bring_scratch(n_z, n_tp, n_gl, w_shape, x_shape, c_shape)
    dma = pltpu.SemaphoreType.DMA
    gate_own, up_own, down_own, mixed = pl.pallas_call(
        functools.partial(whole_kernel, n_z, n_tp, n_gl, len(for_bring)),
        out_shape=(
            jax.ShapeDtypeStruct((n_fs, gate_rows, ffq), bf16),
            jax.ShapeDtypeStruct((n_fs, gate_rows, ffq), bf16),
            jax.ShapeDtypeStruct((share, down_rows, n_tp * cols), bf16),
            jax.ShapeDtypeStruct((tok * n_tp, cols), bf16),
        ),
        in_specs=[hbm] + [vmem] * 3 + [hbm] * 3,
        out_specs=(hbm, hbm, hbm, vmem),
        scratch_shapes=[
            pltpu.VMEM(w_shape, bf16),
            pltpu.VMEM(x_shape, bf16),
            pltpu.VMEM(c_shape, bf16),
            pltpu.VMEM((slots, 2, gate_rows, ffq), f32),
            pltpu.VMEM((slots, 2, gate_rows, ffq), f32),
            pltpu.VMEM((slots, 2, down_rows, cols), f32),
            dma((slots, 3)),
            dma(()),
            dma((2 + n_tp,)),
        ]
        + for_bring
        + apply_scratch(n_z, n_tp, n_fs, tok, d),
        compiler_params=pltpu.CompilerParams(
            collective_id=0, has_side_effects=True, vmem_limit_bytes=67043328
        ),
    )(prompt, routes.T, route_weight.T, norm_gain[None, :], gate_train, up_train, down_train)
    results = (gate_own, up_own, down_own, mixed)
    gate_own, up_own, down_own, mixed = pl.pallas_call(
        hand_over,
        out_shape=tuple(jax.ShapeDtypeStruct(a.shape, a.dtype) for a in results),
        in_specs=[hbm] * 4,
        out_specs=[hbm] * 4,
        scratch_shapes=[pltpu.VMEM(a.shape, a.dtype) for a in results] + [dma((4, 2)), dma((4, 2))],
        compiler_params=pltpu.CompilerParams(vmem_limit_bytes=67043328),
    )(*results)
    return (
        gate_own.reshape(1, d, ffq),
        up_own.reshape(1, d, ffq),
        down_own.reshape(1, share * down_rows, n_tp * cols),
        mixed,
    )


def solution(mesh):
    groups, n_tp = mesh.shape["grp"], mesh.shape["tp"]
    chips = mesh.shape["fs"] // 2
    pair = 2 if groups % 2 == 0 else 1
    finer = Mesh(
        mesh.devices.reshape(groups // pair, pair, chips, 2, n_tp),
        ("gh", "gl", "z", "core", "tp"),
    )
    return jax.shard_map(
        shards,
        mesh=finer,
        in_specs=(P(ROWS), P(ROWS), P(ROWS), P(FS), P(None, FS, "tp"), P(None, FS, "tp"), P(None, FS, "tp")),
        out_specs=(P(ROWS, None, "tp"), P(ROWS, None, "tp"), P(ROWS, "tp", None), P(ROWS, "tp")),
        check_vma=False,
    )
```
